32 devices in a mesh: grp: 2 (over y), ep: 4 (over z), tp: 4 (over x, core).
Axes of the slice: x: 2, y: 2, z: 4, core: 2. Of those that a mesh axis runs over, the one named last changes fastest.
Arguments:
- queries: bfloat16 [3072, 1024], P(('grp', 'ep'), 'tp'), parts along dimension 0, may hold values from -6 to 6
- key_values: bfloat16 [3072, 512], P(('grp', 'ep'), 'tp'), parts along dimension 0, may hold values from -6 to 6
- query_gain: float32 [64], replicated, may hold values from 0.5 to 5
- key_gain: float32 [64], replicated, may hold values from 0.5 to 5
- out_weight: bfloat16 [1024, 2048], P('tp'), may hold values from -0.1875 to 0.1875
- second_batch: bfloat16 [4096, 2048], P(('grp', 'ep', 'tp')), parts along dimension 0, may hold values from -6 to 6
- norm_gain: float32 [2048], replicated, may hold values from 0.1 to 1.9
- routes: int32 [4096, 2], P(('grp', 'ep', 'tp')), parts along dimension 0, may hold values from 0 to 7, all different within a row; in each aligned block of 128 rows (0 to 127, 128 to 255, ...) at most 48 rows name the same one
- route_weights: float32 [4096, 2], P(('grp', 'ep', 'tp')), parts along dimension 0, may hold values from 0.2 to 1
- expert_gate: bfloat16 [8, 2048, 1024], P('ep', None, 'tp'), may hold values from -0.125 to 0.125
- expert_up: bfloat16 [8, 2048, 1024], P('ep', None, 'tp'), may hold values from -0.125 to 0.125
- expert_down: bfloat16 [8, 1024, 2048], P('ep', 'tp'), may hold values from -0.1875 to 0.1875
- shared_gate: bfloat16 [2048, 512], P(None, 'tp'), may hold values from -0.125 to 0.125
- shared_up: bfloat16 [2048, 512], P(None, 'tp'), may hold values from -0.125 to 0.125
- shared_down: bfloat16 [512, 2048], P('tp'), may hold values from -0.25 to 0.25
Outputs:
- mixer_out: bfloat16 [3072, 2048], P(('grp', 'ep', 'tp')), parts along dimension 0
- channel_out: bfloat16 [4096, 2048], P(('grp', 'ep', 'tp')), parts along dimension 0
The draws below stay inside these ranges and needn't reach their ends.
There are 2 independent parts, one for each index of `grp`. The reference program is written for one: setup_inputs(seed, part) draws one part's arguments, and reference() takes and returns one part's arrays. A program takes and returns all parts, laid end to end along the dimension named above; an argument that names none is the same for every part. Nothing has to cross between parts.
Inputs may be any that keep to these rules, and one draw needn't show every extreme that they name: `routes`: each row names 2 different experts. Among the rows of one device no expert is named more than 48 times, and in every draw some expert is named exactly 48 times by the rows of some device.
All inputs are finite; a program needn't handle non-finite values.
Results may differ from the reference program's by a relative error of at most 0.015.
The reference program's roundings to bfloat16 on the way count: a program that leaves them out, or rounds other values in their place, can miss the bound.
Values may be sent and summed in bfloat16 or wider, within the bound.
No kernel may reach another device: no remote copies, remote signals or barrier semaphores. Data moves between devices by JAX's collectives and lax.ppermute only.
A program may use at most 128 MiB of HBM per device.

```python
import math
import jax
import jax.numpy as jnp
import numpy as np
from jax import lax

D = 2048
HEAD = 64
HQ_DEV = 4
HQ = 16
KV_HEADS = 4
GRID_W = 64
TOK_A = 384
TOKENS_A = 1536
TOK_B = 128
TOKENS_B = 2048
TOP_K = 2
EXPERTS = 8
FE_DEV = 256
EXPERT_HIDDEN = 1024
SH_DEV = 128
SHARED = 512
CAP = 48
N_EP = 4


def draw_base(key):
    keyvals = jnp.clip(jax.random.normal(jax.random.fold_in(key, 71), (TOKENS_A, KV_HEADS, 2 * HEAD), jnp.float32), -6.0, 6.0)
    queries = jnp.clip(jax.random.normal(jax.random.fold_in(key, 72), (TOKENS_A, HQ, HEAD), jnp.float32), -6.0, 6.0)
    return (queries.reshape(TOKENS_A, HQ * HEAD), keyvals.reshape(TOKENS_A, KV_HEADS * 2 * HEAD))


def draw_queries(key, part):
    return draw_base(key)[0].astype(jnp.bfloat16)


def draw_key_values(key, part):
    return draw_base(key)[1].astype(jnp.bfloat16)


def draw_gain_common(key, salt):
    return 1.0 + 0.18 * jnp.clip(jax.random.normal(jax.random.fold_in(key, salt + 1), (HEAD,), jnp.float32), -2.5, 2.5)


def draw_query_gain(key, part):
    return draw_gain_common(key, 81)


def draw_key_gain(key, part):
    return draw_gain_common(key, 91)


def block_scale(own_key, dims, pieces, low, top_value):
    def one(axis_at, shards_of):
        heights = jax.random.uniform(jax.random.fold_in(jax.random.fold_in(own_key, 6), axis_at), (shards_of,), jnp.float32, low / len(pieces), top_value / len(pieces))
        return jnp.repeat(jnp.exp(heights), dims[axis_at] // shards_of).reshape((-1,) + (1,) * (len(dims) - axis_at - 1))

    level = one(*pieces[0])
    for cut in pieces[1:]:
        level = level * one(*cut)
    return level


def assign_block(rng, own, number, rows, amount, top, reach, slope):
    ranking = jax.random.permutation(rng, amount)
    packed, ordinary = shares(amount, rows * top, reach, slope, True), shares(amount, rows * top, reach, slope, False)
    places = jnp.arange(amount)

    def named(lengths, rotation):
        used = int((lengths > 0).sum())
        fixed = max(1, used // 4)
        passed = fixed + (places - fixed + rotation * (used - fixed)) % max(1, amount - fixed)
        return jnp.zeros((amount,), jnp.int32).at[ranking[jnp.where(places < fixed, places, passed)]].set(jnp.asarray(lengths, jnp.int32))

    lengths = jnp.where(number % 4 == 0, named(packed, number // 4), named(ordinary, number - number // 4 - 1))
    mixed = jax.random.permutation(jax.random.fold_in(own, 3), amount)
    source_of, sink = mixed[0:amount // 2 * 2:2], mixed[1:amount // 2 * 2:2]
    room = jnp.minimum(lengths[source_of] - 1, reach - lengths[sink]) // 2
    room = jnp.where((source_of == ranking[0]) | (sink == ranking[0]) | (lengths[sink] == 0), 0, jnp.maximum(room, 0))
    passed = jax.random.randint(jax.random.fold_in(own, 4), (amount // 2,), 0, 1 << 20) % (room + 1)
    lengths = lengths.at[source_of].add(-passed).at[sink].add(passed)
    items = jnp.searchsorted(jnp.cumsum(lengths), jnp.arange(rows * top), side="right").astype(jnp.int32)
    grid = items.reshape(top, rows).T
    grid = grid[jax.random.permutation(jax.random.fold_in(own, 1), rows)]
    rotation = jax.random.randint(jax.random.fold_in(own, 2), (rows, 1), 0, top)
    return jnp.take_along_axis(grid, (jnp.arange(top)[None, :] + rotation) % top, axis=1)


def shares(amount, total, bound, skew, full):
    loads = [(1 << 20) // math.isqrt(rank ** skew) + 1 for rank in range(1, amount + 1)]
    largest = bound if full else min(bound, max(-(-total // amount), total * loads[0] // sum(loads)))
    least = 1 if total - largest >= amount - 1 else 0
    holding, surplus = [largest] + [least] * (amount - 1), total - largest - least * (amount - 1)
    while surplus > 0:
        candidates = [i for i in range(1, amount) if holding[i] < largest] or [i for i in range(1, amount) if holding[i] < bound]
        mass, budget = sum([loads[i] for i in candidates]), surplus
        for i in candidates:
            extra = min(bound - holding[i], max(1, budget * loads[i] // mass), surplus)
            holding[i] = holding[i] + extra
            surplus = surplus - extra
    return np.array(holding)


def centred(key, extent, width, bound, split=(), held_as=jnp.bfloat16):
    factor_of = block_scale(key, extent, split, -0.22, 0.18) if split else 1.0
    entries = jax.random.normal(key, extent, jnp.float32) * width * factor_of
    return jnp.minimum(jnp.maximum(entries, -bound), bound).astype(held_as)


def setup_inputs(seed: int = 0, part: int = 0) -> dict:
    arg_keys = jax.random.split(jax.random.key(seed), 16)
    own_keys = jax.random.split(jax.random.fold_in(arg_keys[15], part), 16)
    queries = draw_queries(jax.random.fold_in(jax.random.fold_in(arg_keys[15], part), 71), part)
    key_values = draw_key_values(jax.random.fold_in(jax.random.fold_in(arg_keys[15], part), 71), part)
    query_gain = draw_query_gain(jax.random.fold_in(arg_keys[15], 71), part)
    key_gain = draw_key_gain(jax.random.fold_in(arg_keys[15], 71), part)
    out_weight = centred(arg_keys[4], (HQ * HEAD, D), (HQ * HEAD) ** -0.5, 0.1875, ((0, 4),))
    second_batch = centred(own_keys[5], (TOKENS_B, D), 1.0, 6.0, ((0, 16),))
    norm_gain = jnp.clip(1.0 + 0.18 * jax.random.normal(arg_keys[6], (D,), jnp.float32), 0.1, 1.9)
    routes_keys = jax.random.split(jax.random.fold_in(own_keys[7], 1), TOKENS_B // TOK_B)
    routes_turns = jax.random.permutation(jax.random.fold_in(own_keys[7], 3), TOKENS_B // TOK_B)
    routes = jax.vmap(lambda own, number: assign_block(jax.random.fold_in(own_keys[7], 2), own, number, TOK_B, EXPERTS, TOP_K, CAP, 2))(routes_keys, routes_turns).reshape((TOKENS_B, TOP_K))
    route_weights = jnp.clip(0.2 + 0.8 * jax.random.uniform(own_keys[8], (TOKENS_B, TOP_K), jnp.float32) ** block_scale(own_keys[8], (TOKENS_B, TOP_K), ((0, 16),), -0.2, 0.2), 0.2, 1.0)
    expert_gate = centred(arg_keys[9], (EXPERTS, D, EXPERT_HIDDEN), D ** -0.5, 0.125, ((0, 4), (2, 4)))
    expert_up = centred(arg_keys[10], (EXPERTS, D, EXPERT_HIDDEN), D ** -0.5, 0.125, ((0, 4), (2, 4)))
    expert_down = centred(arg_keys[11], (EXPERTS, EXPERT_HIDDEN, D), EXPERT_HIDDEN ** -0.5, 0.1875, ((0, 4), (1, 4)))
    shared_gate = centred(arg_keys[12], (D, SHARED), D ** -0.5, 0.125, ((1, 4),))
    shared_up = centred(arg_keys[13], (D, SHARED), D ** -0.5, 0.125, ((1, 4),))
    shared_down = centred(arg_keys[14], (SHARED, D), SHARED ** -0.5, 0.25, ((0, 4),))
    return dict(queries=queries, key_values=key_values, query_gain=query_gain, key_gain=key_gain, out_weight=out_weight, second_batch=second_batch, norm_gain=norm_gain, routes=routes, route_weights=route_weights, expert_gate=expert_gate, expert_up=expert_up, expert_down=expert_down, shared_gate=shared_gate, shared_up=shared_up, shared_down=shared_down)


rope_base = 10000.0
norm_eps = 1e-06

def head_norm(vectors, gain):
    return vectors * lax.rsqrt(lax.optimization_barrier(jnp.mean(vectors * vectors, axis=-1, keepdims=True)) + norm_eps) * gain

def turn_heads(vectors, positions):
    row_count, head_count, head_size = vectors.shape
    half_size = head_size // 2
    inverse = rope_base ** (-jnp.arange(0, half_size, 2, dtype=jnp.float32) / half_size)
    grid_row = (positions // GRID_W).astype(jnp.float32)
    grid_column = (positions % GRID_W).astype(jnp.float32)
    angles = jnp.concatenate([grid_row[:, None] * inverse, grid_column[:, None] * inverse], axis=-1)
    cosine = jnp.cos(angles)[:, None, :]
    sine = jnp.sin(angles)[:, None, :]
    paired = vectors.reshape(row_count, head_count, half_size, 2)
    first = paired[..., 0]
    second = paired[..., 1]
    turned = jnp.stack([first * cosine - second * sine, first * sine + second * cosine], axis=-1)
    return turned.reshape(vectors.shape)

def slot_ids(route_rows, expert_count, capacity):
    row_count, top_count = route_rows.shape
    flat_routes = route_rows.reshape(-1)
    onehot = (flat_routes[:, None] == jnp.arange(expert_count, dtype=jnp.int32)[None, :]).astype(jnp.int32)
    earlier = (jnp.cumsum(onehot, axis=0).astype(jnp.int32) - onehot).astype(jnp.int32)
    within = lax.optimization_barrier(jnp.sum(earlier * onehot, axis=1)).astype(jnp.int32)
    return (flat_routes * capacity + within).astype(jnp.int32).reshape(row_count, top_count)

def slot_table(slots, slot_count):
    row_count, top_count = slots.shape
    flat_slots = slots.reshape(-1)
    owner_row = jnp.arange(row_count * top_count, dtype=jnp.int32) // top_count
    matches = flat_slots[None, :] == jnp.arange(slot_count, dtype=jnp.int32)[:, None]
    occupied = jnp.any(matches, axis=1)
    source_row = lax.optimization_barrier(jnp.sum(jnp.where(matches, owner_row[None, :], 0), axis=1)).astype(jnp.int32)
    return jnp.where(occupied, source_row, row_count).astype(jnp.int32)

def block_sum(hidden, down_weights, block_width):
    summed = jnp.zeros((hidden.shape[0], down_weights.shape[1]), jnp.float32)
    for block_index in range(hidden.shape[1] // block_width):
        lower = block_index * block_width
        partial_value = jnp.dot(hidden[:, lower:lower + block_width], down_weights[lower:lower + block_width], preferred_element_type=jnp.float32).astype(jnp.bfloat16)
        summed = summed + lax.optimization_barrier(partial_value).astype(jnp.float32)
    return summed

def swiglu_hidden(token_rows, gate_weights, up_weights):
    gate_part = jnp.dot(token_rows, gate_weights, preferred_element_type=jnp.float32)
    up_part = jnp.dot(token_rows, up_weights, preferred_element_type=jnp.float32)
    return (jax.nn.silu(gate_part) * up_part).astype(jnp.bfloat16)

def expert_apply(operands):
    slot_rows, gate_weights, up_weights, down_weights = operands
    hidden = swiglu_hidden(slot_rows, gate_weights, up_weights)
    return block_sum(hidden, down_weights, FE_DEV).astype(jnp.bfloat16)

def reference(queries, key_values, query_gain, key_gain, out_weight, second_batch, norm_gain, routes, route_weights, expert_gate, expert_up, expert_down, shared_gate, shared_up, shared_down):
    total_rows = queries.shape[0]
    positions = jnp.arange(total_rows, dtype=jnp.int32)
    query_turned = turn_heads(head_norm(queries.reshape(total_rows, HQ, HEAD).astype(jnp.float32), query_gain), positions).astype(jnp.bfloat16)
    query_turned = lax.optimization_barrier(query_turned)
    pairs = key_values.reshape(total_rows, KV_HEADS, 2 * HEAD)
    key_turned = turn_heads(head_norm(pairs[:, :, :HEAD].astype(jnp.float32), key_gain), positions).astype(jnp.bfloat16)
    key_float = lax.optimization_barrier(key_turned).astype(jnp.float32)
    value_float = pairs[:, :, HEAD:].astype(jnp.float32)
    scale = HEAD ** (-0.5)

    def query_block(block_queries):
        summed = jnp.zeros((block_queries.shape[0], D), jnp.float32)
        for head_group in range(KV_HEADS):
            group_queries = block_queries[:, head_group * HQ_DEV:(head_group + 1) * HQ_DEV].astype(jnp.float32)
            scores = jnp.einsum('qhd,kd->hqk', group_queries, key_float[:, head_group]) * scale
            top = lax.optimization_barrier(jnp.max(scores, axis=-1, keepdims=True))
            exps = jnp.exp(scores - top)
            totals = lax.optimization_barrier(jnp.sum(exps, axis=-1))
            weights = lax.optimization_barrier(exps.astype(jnp.bfloat16)).astype(jnp.float32)
            numerators = jnp.einsum('hqk,kd->qhd', weights, value_float[:, head_group])
            head_out = (numerators / totals.T[:, :, None]).astype(jnp.bfloat16).reshape(-1, HQ_DEV * HEAD)
            lower = head_group * HQ_DEV * HEAD
            partial_value = jnp.dot(head_out, out_weight[lower:lower + HQ_DEV * HEAD], preferred_element_type=jnp.float32).astype(jnp.bfloat16)
            summed = summed + lax.optimization_barrier(partial_value).astype(jnp.float32)
        return summed.astype(jnp.bfloat16)
    mixer_out = lax.map(query_block, query_turned.reshape(N_EP, TOK_A, HQ, HEAD)).reshape(total_rows, D)
    token_float = second_batch.astype(jnp.float32)
    normed = (token_float * lax.rsqrt(lax.optimization_barrier(jnp.mean(token_float * token_float, axis=-1, keepdims=True)) + norm_eps) * norm_gain).astype(jnp.bfloat16)
    block_count = normed.shape[0] // TOK_B
    slot_count = EXPERTS * CAP
    slots = jax.vmap(lambda route_rows: slot_ids(route_rows, EXPERTS, CAP))(routes.reshape(block_count, TOK_B, TOP_K))
    tables = jax.vmap(lambda slot_block: slot_table(slot_block, slot_count))(slots)
    inputs = jax.vmap(lambda token_rows, table_rows: jnp.take(token_rows, table_rows, axis=0, mode='fill', fill_value=0))(normed.reshape(block_count, TOK_B, D), tables)
    per_expert = inputs.reshape(block_count, EXPERTS, CAP, D).transpose(1, 0, 2, 3).reshape(EXPERTS, block_count * CAP, D)
    outputs = lax.map(expert_apply, (per_expert, expert_gate, expert_up, expert_down))
    by_block = outputs.reshape(EXPERTS, block_count, CAP, D).transpose(1, 0, 2, 3).reshape(block_count, slot_count, D)
    chosen = jax.vmap(lambda block_out, slot_block: jnp.take(block_out, slot_block.reshape(-1), axis=0))(by_block, slots).reshape(-1, TOP_K, D)
    routed = lax.optimization_barrier(jnp.sum(route_weights[:, :, None] * chosen.astype(jnp.float32), axis=1))
    shared_hidden = swiglu_hidden(normed, shared_gate, shared_up)
    shared_sum = block_sum(shared_hidden, shared_down, SH_DEV)
    channel_out = (shared_sum + routed).astype(jnp.bfloat16)
    return (mixer_out, channel_out)
```

```python
import functools

import jax
import jax.numpy as jnp
from jax import lax
from jax.experimental import pallas as pl
from jax.experimental.pallas import tpu as pltpu
from jax.sharding import PartitionSpec as P


GRID_W = 64


rope_base = 10000.0
norm_eps = 1e-06


def head_norm(vectors, gain):
    return (
        vectors * lax.rsqrt(jnp.mean(vectors * vectors, axis=-1, keepdims=True) + norm_eps) * gain
    )


def turn_heads(vectors, positions):
    row_count, head_count, head_size = vectors.shape
    half_size = head_size // 2
    inverse = rope_base ** (-jnp.arange(0, half_size, 2, dtype=jnp.float32) / half_size)
    grid_row = (positions // GRID_W).astype(jnp.float32)
    grid_column = (positions % GRID_W).astype(jnp.float32)
    angles = jnp.concatenate([grid_row[:, None] * inverse, grid_column[:, None] * inverse], axis=-1)
    cosine = jnp.cos(angles)[:, None, :]
    sine = jnp.sin(angles)[:, None, :]
    paired = vectors.reshape(row_count, head_count, half_size, 2)
    first = paired[..., 0]
    second = paired[..., 1]
    turned = jnp.stack([first * cosine - second * sine, first * sine + second * cosine], axis=-1)
    return turned.reshape(vectors.shape)


def slot_ids(route_rows, expert_count, capacity):
    row_count, top_count = route_rows.shape
    flat_routes = route_rows.reshape(-1)
    onehot = (flat_routes[:, None] == jnp.arange(expert_count, dtype=jnp.int32)[None, :]).astype(
        jnp.int32
    )
    earlier = jnp.cumsum(onehot, axis=0) - onehot
    within = jnp.sum(earlier * onehot, axis=1)
    return (flat_routes * capacity + within).reshape(row_count, top_count)


def slot_table(slots, slot_count):
    row_count, top_count = slots.shape
    flat_slots = slots.reshape(-1)
    owner_row = jnp.arange(row_count * top_count, dtype=jnp.int32) // top_count
    matches = flat_slots[None, :] == jnp.arange(slot_count, dtype=jnp.int32)[:, None]
    occupied = jnp.any(matches, axis=1)
    source_row = jnp.sum(jnp.where(matches, owner_row[None, :], 0), axis=1)
    return jnp.where(occupied, source_row, row_count)


def pick_block(row_count):
    for candidate in range(min(row_count, 1024), 0, -1):
        if row_count % candidate == 0:
            return candidate
    return row_count


def attend_keys(query_turned, scale, running, pieces):
    head_size = query_turned.shape[-1]
    key_block = pick_block(pieces.shape[0])
    blocks = pieces.reshape(pieces.shape[0] // key_block, key_block, 2 * head_size)

    def one_block(carried, block_rows):
        top_now, total_now, acc_now = carried
        scores = (
            jnp.einsum(
                "qhd,kd->hqk",
                query_turned,
                block_rows[:, :head_size],
                preferred_element_type=jnp.float32,
            )
            * scale
        )
        top_new = jnp.maximum(top_now, jnp.max(scores, axis=-1))
        shrink = jnp.exp(top_now - top_new)
        exps = jnp.exp(scores - top_new[..., None])
        total_new = total_now * shrink + jnp.sum(exps, axis=-1)
        acc_new = acc_now * shrink[..., None] + jnp.einsum(
            "hqk,kd->hqd",
            exps.astype(jnp.bfloat16),
            block_rows[:, head_size:],
            preferred_element_type=jnp.float32,
        )
        return ((top_new, total_new, acc_new), None)

    result, ignored = lax.scan(one_block, running, blocks)
    return result


def shared_hidden_of(token_rows, gate_weights, up_weights):
    gate_part = jnp.dot(token_rows, gate_weights, preferred_element_type=jnp.float32)
    up_part = jnp.dot(token_rows, up_weights, preferred_element_type=jnp.float32)
    return (jax.nn.silu(gate_part) * up_part).astype(jnp.bfloat16)


def expert_hidden(slot_rows, gate_weights, up_weights):
    gate_part = jnp.einsum(
        "osjcd,jdf->osjcf", slot_rows, gate_weights, preferred_element_type=jnp.float32
    )
    up_part = jnp.einsum(
        "osjcd,jdf->osjcf", slot_rows, up_weights, preferred_element_type=jnp.float32
    )
    return (jax.nn.silu(gate_part) * up_part).astype(jnp.bfloat16)


def body_slots(
    queries,
    key_values,
    query_gain,
    key_gain,
    out_weight,
    second_batch,
    norm_gain,
    routes,
    route_weights,
    expert_gate,
    expert_up,
    expert_down,
    shared_gate,
    shared_up,
    shared_down,
):
    query_rows = queries.shape[0]
    head_size = query_gain.shape[0]
    heads_here = queries.shape[1] // head_size
    ep_count = lax.axis_size("ep")
    positions = lax.axis_index("ep") * query_rows + jnp.arange(query_rows, dtype=jnp.int32)
    query_turned = turn_heads(
        head_norm(
            queries.reshape(query_rows, heads_here, head_size).astype(jnp.float32), query_gain
        ),
        positions,
    ).astype(jnp.bfloat16)
    key_turned = turn_heads(
        head_norm(key_values[:, None, :head_size].astype(jnp.float32), key_gain), positions
    ).astype(jnp.bfloat16)
    keys_and_values = jnp.concatenate([key_turned[:, 0, :], key_values[:, head_size:]], axis=1)
    start_state = (
        jnp.full((heads_here, query_rows), -1e30, jnp.float32),
        jnp.zeros((heads_here, query_rows), jnp.float32),
        jnp.zeros((heads_here, query_rows, head_size), jnp.float32),
    )
    top_all, total_all, acc_all = attend_keys(
        query_turned,
        head_size ** (-0.5),
        start_state,
        lax.all_gather(keys_and_values, "ep", axis=0, tiled=True),
    )
    head_out = (
        (acc_all / total_all[..., None])
        .transpose(1, 0, 2)
        .reshape(query_rows, heads_here * head_size)
        .astype(jnp.bfloat16)
    )
    tok_count = second_batch.shape[0]
    model_width = second_batch.shape[1]
    top_count = routes.shape[1]
    local_experts = expert_gate.shape[0]
    expert_count = local_experts * ep_count
    capacity = 3 * tok_count * top_count // (2 * expert_count)
    slot_count = expert_count * capacity
    token_float = second_batch.astype(jnp.float32)
    normed = (
        token_float
        * lax.rsqrt(jnp.mean(token_float * token_float, axis=-1, keepdims=True) + norm_eps)
        * norm_gain
    ).astype(jnp.bfloat16)
    own_slots = slot_ids(routes, expert_count, capacity)
    shared_hidden = shared_hidden_of(
        lax.all_gather(normed, "tp", axis=0, tiled=True), shared_gate, shared_up
    )
    outgoing = jnp.take(
        normed, slot_table(own_slots, slot_count), axis=0, mode="fill", fill_value=0
    )[None]
    arrived = lax.all_to_all(outgoing, "ep", split_axis=1, concat_axis=1, tiled=True)
    arrived = arrived.reshape(arrived.shape[0], ep_count, local_experts, capacity, model_width)
    hidden = expert_hidden(
        lax.all_gather(arrived, "tp", axis=0, tiled=True), expert_gate, expert_up
    )
    routed_part = jnp.einsum(
        "osjcf,jfd->osjcd", hidden, expert_down, preferred_element_type=jnp.float32
    ).reshape(-1, model_width)
    shared_part = jnp.dot(shared_hidden, shared_down, preferred_element_type=jnp.float32)
    head_partial = jnp.dot(head_out, out_weight, preferred_element_type=jnp.float32)
    attn_sum, routed_sum, shared_sum = (
        lax.psum_scatter(
            head_partial.astype(jnp.bfloat16), "tp", scatter_dimension=0, tiled=True
        ).astype(jnp.float32),
        lax.psum_scatter(
            routed_part.astype(jnp.bfloat16), "tp", scatter_dimension=0, tiled=True
        ).astype(jnp.float32),
        lax.psum_scatter(
            shared_part.astype(jnp.bfloat16), "tp", scatter_dimension=0, tiled=True
        ).astype(jnp.float32),
    )
    returned = lax.all_to_all(
        routed_sum.astype(jnp.bfloat16), "ep", split_axis=0, concat_axis=0, tiled=True
    )
    combined = shared_sum
    for slot_pick in range(top_count):
        combined = combined + route_weights[:, slot_pick : slot_pick + 1] * jnp.take(
            returned, own_slots[:, slot_pick], axis=0
        ).astype(jnp.float32)
    return (attn_sum.astype(jnp.bfloat16), combined.astype(jnp.bfloat16))


def angle_tables(positions, head_size):
    half_size = head_size // 2
    inverse = rope_base ** (-jnp.arange(0, half_size, 2, dtype=jnp.float32) / half_size)
    grid_row = (positions // GRID_W).astype(jnp.float32)
    grid_column = (positions % GRID_W).astype(jnp.float32)
    angles = jnp.concatenate([grid_row[:, None] * inverse, grid_column[:, None] * inverse], axis=-1)
    angles = jnp.repeat(angles, 2, axis=-1)
    sign = jnp.where(jnp.arange(head_size) % 2 == 0, -1.0, 1.0)
    return jnp.cos(angles), jnp.sin(angles) * sign


def norm_turn(vectors, gain, cosine, sine):
    width = vectors.shape[-1]
    scaled = (
        vectors * lax.rsqrt(jnp.mean(vectors * vectors, axis=-1, keepdims=True) + norm_eps) * gain
    )
    lane = lax.broadcasted_iota(jnp.int32, scaled.shape, 1)
    doubled = jnp.concatenate([scaled, scaled], axis=-1)
    after = pltpu.roll(doubled, 2 * width - 1, 1)[:, :width]
    before = pltpu.roll(doubled, 1, 1)[:, :width]
    swapped = jnp.where(lane % 2 == 0, after, before)
    return scaled * cosine + swapped * sine


def turn_kernel(heads, head_size, q_ref, kv_ref, qg_ref, kg_ref, cos_ref, sin_ref, q_out, kv_out):
    cosine = cos_ref[...]
    sine = sin_ref[...]
    for head in range(heads):
        part = slice(head * head_size, (head + 1) * head_size)
        q_out[:, part] = norm_turn(
            q_ref[:, part].astype(jnp.float32), qg_ref[...], cosine, sine
        ).astype(jnp.bfloat16)
    kv_out[:, :head_size] = norm_turn(
        kv_ref[:, :head_size].astype(jnp.float32), kg_ref[...], cosine, sine
    ).astype(jnp.bfloat16)
    kv_out[:, head_size:] = kv_ref[:, head_size:]


def attend_kernel(heads, head_size, pieces, q_ref, *refs):
    kv_refs = refs[:pieces]
    out_ref = refs[pieces]
    scale = head_size ** (-0.5)
    keys_values = jnp.concatenate([ref[...] for ref in kv_refs], axis=0)
    keys = keys_values[:, :head_size]
    values = keys_values[:, head_size:]
    for head in range(heads):
        part = slice(head * head_size, (head + 1) * head_size)
        scores = (
            lax.dot_general(
                q_ref[:, part],
                keys,
                (((1,), (1,)), ((), ())),
                preferred_element_type=jnp.float32,
            )
            * scale
        )
        exps = jnp.exp(scores - jnp.max(scores, axis=-1, keepdims=True))
        totals = jnp.sum(exps, axis=-1, keepdims=True)
        mixed = jnp.dot(exps.astype(jnp.bfloat16), values, preferred_element_type=jnp.float32)
        out_ref[:, part] = (mixed / totals).astype(jnp.bfloat16)


def swish_times(gate_part, up_part):
    return gate_part / (1.0 + jnp.exp(-gate_part)) * up_part


def expert_kernel(block_count, local_experts, with_shared, *refs):
    refs = list(refs)
    first_ref = refs.pop(0)
    tokens = [refs.pop(0) for _ in range(block_count)]
    routing = [refs.pop(0) for _ in range(block_count)]
    gain_ref = refs.pop(0)
    gates = [refs.pop(0) for _ in range(2)]
    ups = [refs.pop(0) for _ in range(2)]
    downs = [refs.pop(0) for _ in range(2)]
    if with_shared:
        sgates = [refs.pop(0) for _ in range(2)]
        sups = [refs.pop(0) for _ in range(2)]
        sdowns = [refs.pop(0) for _ in range(2)]
    outs = [refs.pop(0) for _ in range(block_count)]
    gate_buf, up_buf, down_buf, hidden_buf, normed_buf, sems = refs[:6]
    width = gates[0].shape[2]
    rows = tokens[0].shape[0]
    copies = []
    steps = [(s, j) for s in range(2) for j in range(local_experts)]
    for n, (s, j) in enumerate(steps):
        copies.append(
            (
                pltpu.make_async_copy(gates[s].at[j], gate_buf.at[n], sems.at[n, 0]),
                pltpu.make_async_copy(ups[s].at[j], up_buf.at[n], sems.at[n, 1]),
            )
        )
    down_copies = [
        pltpu.make_async_copy(
            downs[s].at[j], down_buf.at[pl.ds(n * width, width)], sems.at[n, 2]
        )
        for n, (s, j) in enumerate(steps)
    ]
    for pair in copies:
        pair[0].start()
        pair[1].start()
    for copy in down_copies:
        copy.start()
    gain = gain_ref[...]
    columns = []
    expert_total = routing[0].shape[0] // 2
    for b in range(block_count):
        token_float = tokens[b][...].astype(jnp.float32)
        normed_buf[b * rows : (b + 1) * rows] = (
            token_float
            * lax.rsqrt(jnp.mean(token_float * token_float, axis=-1, keepdims=True) + norm_eps)
            * gain
        ).astype(jnp.bfloat16)
        both = routing[b][...].astype(jnp.float32)
        columns.append((both[:expert_total] + both[expert_total:]).T)
    weights = jnp.concatenate(columns, axis=0)
    lane = lax.broadcasted_iota(jnp.int32, weights.shape, 1)
    first = first_ref[0]
    for n, (s, j) in enumerate(steps):
        copies[n][0].wait()
        copies[n][1].wait()
        column = jnp.sum(jnp.where(lane == first + j, weights, 0.0), axis=1, keepdims=True)
        gate_part = jnp.dot(normed_buf[...], gate_buf[n], preferred_element_type=jnp.float32)
        up_part = jnp.dot(normed_buf[...], up_buf[n], preferred_element_type=jnp.float32)
        hidden_buf[:, n * width : (n + 1) * width] = (
            swish_times(gate_part, up_part) * column
        ).astype(jnp.bfloat16)
    for copy in down_copies:
        copy.wait()
    total = jnp.dot(hidden_buf[...], down_buf[...], preferred_element_type=jnp.float32)
    if with_shared:
        for s in range(2):
            normed = normed_buf[: with_shared * rows]
            gate_part = jnp.dot(normed, sgates[s][...], preferred_element_type=jnp.float32)
            up_part = jnp.dot(normed, sups[s][...], preferred_element_type=jnp.float32)
            shared = jnp.dot(
                swish_times(gate_part, up_part).astype(jnp.bfloat16),
                sdowns[s][...],
                preferred_element_type=jnp.float32,
            )
            if with_shared == block_count:
                total = total + shared
            else:
                total = jnp.concatenate(
                    [total[: with_shared * rows] + shared, total[with_shared * rows :]], axis=0
                )
    for b in range(block_count):
        outs[b][...] = total[b * rows : (b + 1) * rows].astype(jnp.bfloat16)


def run_experts(first, blocks, routing, gain, gates, ups, downs, shared=None, with_shared=0):
    count = len(blocks)
    rows, depth = blocks[0].shape
    local_experts, _, width = gates[0].shape
    total_hidden = 2 * local_experts * width
    vmem = pl.BlockSpec(memory_space=pltpu.VMEM)
    anywhere = pl.BlockSpec(memory_space=pl.ANY)
    operands = [first, *blocks, *routing, gain, *gates, *ups, *downs]
    specs = [pl.BlockSpec(memory_space=pltpu.SMEM)] + [vmem] * (2 * count + 1) + [anywhere] * 6
    if with_shared:
        operands += [*shared[0], *shared[1], *shared[2]]
        specs += [vmem] * 6
    flops = 2 * count * rows * depth * total_hidden * 3
    return pl.pallas_call(
        functools.partial(expert_kernel, count, local_experts, with_shared),
        out_shape=[jax.ShapeDtypeStruct((rows, depth), jnp.bfloat16)] * count,
        in_specs=specs,
        out_specs=[vmem] * count,
        scratch_shapes=[
            pltpu.VMEM((2 * local_experts, depth, width), jnp.bfloat16),
            pltpu.VMEM((2 * local_experts, depth, width), jnp.bfloat16),
            pltpu.VMEM((total_hidden, depth), jnp.bfloat16),
            pltpu.VMEM((count * rows, total_hidden), jnp.bfloat16),
            pltpu.VMEM((count * rows, depth), jnp.bfloat16),
            pltpu.SemaphoreType.DMA((2 * local_experts, 3)),
        ],
        compiler_params=pltpu.CompilerParams(vmem_limit_bytes=48 * 1024 * 1024),
        cost_estimate=pl.CostEstimate(
            flops=flops, transcendentals=0, bytes_accessed=6 * depth * total_hidden
        ),
    )(*operands)


def body_dense(
    queries,
    key_values,
    query_gain,
    key_gain,
    out_weight,
    second_batch,
    norm_gain,
    routes,
    route_weights,
    expert_gate,
    expert_up,
    expert_down,
    shared_gate,
    shared_up,
    shared_down,
):
    query_rows = queries.shape[0]
    head_size = query_gain.shape[0]
    heads_here = queries.shape[1] // head_size
    ep_count = lax.axis_size("ep")
    tp_count = lax.axis_size("tp")
    ep_index = lax.axis_index("ep")
    tp_index = lax.axis_index("tp")
    local_experts = expert_gate.shape[0]
    expert_total = local_experts * ep_count
    vmem = pl.BlockSpec(memory_space=pltpu.VMEM)

    def core_swap(value):
        return lax.ppermute(value, "tp", [(i, i ^ 1) for i in range(tp_count)])

    def pair_swap(value):
        return lax.ppermute(value, "tp", [(i, i ^ 2) for i in range(tp_count)])

    def ring(value, shift=1):
        return lax.ppermute(value, "ep", [(i, (i + shift) % ep_count) for i in range(ep_count)])

    held = [second_batch]
    for hop in range(1, ep_count):
        held.append(ring(held[-1]))
    across = [pair_swap(block) for block in held]

    one_hot = routes[:, :, None] == jnp.arange(expert_total, dtype=jnp.int32)
    combine = jnp.sum(jnp.where(one_hot, route_weights[:, :, None], 0.0), axis=1).T
    high = lax.reduce_precision(combine, 8, 7)
    routing_rows = jnp.concatenate([high, combine - high], axis=0).astype(jnp.bfloat16)

    positions = ep_index * query_rows + jnp.arange(query_rows, dtype=jnp.int32)
    cosine, sine = angle_tables(positions, head_size)
    query_turned, keys_and_values = pl.pallas_call(
        functools.partial(turn_kernel, heads_here, head_size),
        out_shape=[
            jax.ShapeDtypeStruct(queries.shape, jnp.bfloat16),
            jax.ShapeDtypeStruct(key_values.shape, jnp.bfloat16),
        ],
        in_specs=[vmem] * 6,
        out_specs=[vmem] * 2,
        cost_estimate=pl.CostEstimate(flops=2000000000, transcendentals=0, bytes_accessed=500000),
    )(queries, key_values, query_gain[None, :], key_gain[None, :], cosine, sine)

    small = jnp.concatenate([keys_and_values, routing_rows], axis=0)
    smalls = [small] + [ring(small, shift) for shift in range(1, ep_count)]
    routing_own = [piece[query_rows:] for piece in smalls]
    routing_across = pair_swap(jnp.concatenate(routing_own, axis=0))
    routing_across = jnp.split(routing_across, ep_count, axis=0)

    gates = (expert_gate, core_swap(expert_gate))
    ups = (expert_up, core_swap(expert_up))
    downs = (expert_down, core_swap(expert_down))
    shared = (
        (shared_gate, core_swap(shared_gate)),
        (shared_up, core_swap(shared_up)),
        (shared_down, core_swap(shared_down)),
    )
    out_weights = (out_weight, core_swap(out_weight))

    head_out = pl.pallas_call(
        functools.partial(attend_kernel, heads_here, head_size, ep_count),
        out_shape=jax.ShapeDtypeStruct(queries.shape, jnp.bfloat16),
        in_specs=[vmem] * (1 + ep_count),
        out_specs=vmem,
        compiler_params=pltpu.CompilerParams(vmem_limit_bytes=48 * 1024 * 1024),
        cost_estimate=pl.CostEstimate(flops=10000000000, transcendentals=0, bytes_accessed=500000),
    )(query_turned, *[piece[:query_rows] for piece in smalls])

    by_owner = head_out.reshape(tp_count // 2, 2, query_rows // tp_count, -1)
    odd_core = tp_index % 2 == 1
    kept = jnp.where(odd_core, by_owner[:, 1], by_owner[:, 0])
    given = core_swap(jnp.where(odd_core, by_owner[:, 0], by_owner[:, 1]))
    far_side = tp_index // 2 == 1

    def project(mine, partner):
        return (
            jnp.dot(mine, out_weights[0], preferred_element_type=jnp.float32)
            + jnp.dot(partner, out_weights[1], preferred_element_type=jnp.float32)
        ).astype(jnp.bfloat16)

    sent = project(
        jnp.where(far_side, kept[0], kept[1]), jnp.where(far_side, given[0], given[1])
    )
    stays = project(
        jnp.where(far_side, kept[1], kept[0]), jnp.where(far_side, given[1], given[0])
    )
    mixer_out = (stays.astype(jnp.float32) + pair_swap(sent).astype(jnp.float32)).astype(
        jnp.bfloat16
    )

    first = (ep_index * local_experts).astype(jnp.int32).reshape(1)
    gain = norm_gain[None, :]

    def experts_of(hop):
        return run_experts(
            first,
            [held[hop], across[hop]],
            [routing_own[hop], routing_across[hop]],
            gain,
            gates,
            ups,
            downs,
            shared if hop == 0 else None,
            2 if hop == 0 else 0,
        )

    moving = None
    for hop in list(range(1, ep_count)) + [0]:
        own_part, far_part = experts_of(hop)
        total = own_part.astype(jnp.float32) + pair_swap(far_part).astype(jnp.float32)
        if moving is not None:
            total = total + moving.astype(jnp.float32)
        total = total.astype(jnp.bfloat16)
        moving = ring(total) if hop else total
    return (mixer_out, moving)


def body(*arguments):
    queries, second_batch, routes, expert_gate = (arguments[i] for i in (0, 5, 7, 9))
    ep_count = lax.axis_size("ep")
    tok_count, top_count = routes.shape
    slot_count = 3 * tok_count * top_count // 2
    dense = lax.axis_size("tp") == 4 and ep_count * tok_count <= 2 * slot_count
    return (body_dense if dense else body_slots)(*arguments)


def solution(mesh):
    placed = (
        P(("grp", "ep"), "tp"),
        P(("grp", "ep"), "tp"),
        P(),
        P(),
        P("tp", None),
        P(("grp", "ep", "tp"), None),
        P(),
        P(("grp", "ep", "tp"), None),
        P(("grp", "ep", "tp"), None),
        P("ep", None, "tp"),
        P("ep", None, "tp"),
        P("ep", "tp", None),
        P(None, "tp"),
        P(None, "tp"),
        P("tp", None),
    )
    return jax.shard_map(
        body,
        mesh=mesh,
        in_specs=placed,
        out_specs=(P(("grp", "ep", "tp"), None), P(("grp", "ep", "tp"), None)),
        check_vma=False,
    )
```
